32 devices in a mesh: grp: 2 (over y), sp: 4 (over z), tp: 4 (over x, core).
Axes of the slice: x: 2, y: 2, z: 4, core: 2. Of those that a mesh axis runs over, the one named last changes fastest.
Arguments:
- hidden_in: bfloat16 [5120, 4096], P(('grp', 'sp'), 'tp'), parts along dimension 0, may hold values from -64 to 64
- norm_gain: float32 [2, 4096], replicated, may hold values from 0.1 to 1.9
- w_pool_in: bfloat16 [2, 4096, 1024], P(None, 'sp', 'tp'), may hold values from -0.09375 to 0.09375
- w_pool_gate: bfloat16 [2, 4096, 1024], P(None, 'sp', 'tp'), may hold values from -0.09375 to 0.09375
- group_mix: bfloat16 [2, 16, 64, 64], replicated, may hold values from -0.75 to 0.75
- w_out: bfloat16 [2, 1024, 4096], P(None, 'sp', 'tp'), may hold values from -0.1875 to 0.1875
Outputs:
- hidden_out: bfloat16 [5120, 4096], P(('grp', 'sp'), 'tp'), parts along dimension 0
The draws below stay inside these ranges and needn't reach their ends.
There are 2 independent parts, one for each index of `grp`. The reference program is written for one: setup_inputs(seed, part) draws one part's arguments, and reference() takes and returns one part's arrays. A program takes and returns all parts, laid end to end along the dimension named above; an argument that names none is the same for every part. Nothing has to cross between parts.
All inputs are finite; a program needn't handle non-finite values.
Results may differ from the reference program's by a relative error of at most 0.012.
Values may be sent and summed in bfloat16 or wider, within the bound.
A program may use at most 64 MiB of HBM per device.

```python
import jax
import jax.numpy as jnp
from jax import lax

D = 4096
DP = 1024
GROUP = 64
GROUPS = 16
LAYERS = 2
TOKENS = 2560


def draw_hidden_in(key, part):
    base_key = jax.random.fold_in(key, 11)
    key_one, key_two = jax.random.split(base_key, 2)
    values = jax.random.normal(key_one, (TOKENS, D), jnp.float32)
    ramp = jnp.arange(D, dtype=jnp.float32) / D
    column_scale = jnp.exp(jnp.log(10.0) * (0.6 * ramp + 0.4 * jax.random.uniform(key_two, (D,), jnp.float32))) * 0.3162
    values = jnp.clip(values * column_scale[None, :], -60.0, 60.0)
    return values.astype(jnp.bfloat16)


def steps_of(key, extent, cuts, low, largest):
    loudness = 1.0
    for dim, parts in cuts:
        steps = jax.random.uniform(jax.random.fold_in(jax.random.fold_in(key, 6), dim), (parts,), jnp.float32, low / len(cuts), largest / len(cuts))
        loudness = loudness * jnp.repeat(jnp.exp(steps), extent[dim] // parts).reshape((-1,) + (1,) * (len(extent) - 1 - dim))
    return loudness


def scatter_about(rng, shape, scale, most, shards=(), kind=jnp.bfloat16):
    array = scale * jax.random.normal(rng, shape, jnp.float32)
    if shards:
        array = array * steps_of(rng, shape, shards, -0.22, 0.18)
    return jnp.clip(array, -most, most).astype(kind)


def setup_inputs(seed: int = 0, part: int = 0) -> dict:
    arg_keys = jax.random.split(jax.random.key(seed), 7)
    own_keys = jax.random.split(jax.random.fold_in(arg_keys[6], part), 7)
    hidden_in = draw_hidden_in(jax.random.fold_in(jax.random.fold_in(arg_keys[6], part), 71), part)
    norm_gain = jnp.clip(1.0 + 0.18 * jax.random.normal(arg_keys[1], (LAYERS, D), jnp.float32), 0.1, 1.9)
    w_pool_in = scatter_about(arg_keys[2], (LAYERS, D, DP), D ** -0.5, 0.09375, ((1, 4), (2, 4)))
    w_pool_gate = scatter_about(arg_keys[3], (LAYERS, D, DP), D ** -0.5, 0.09375, ((1, 4), (2, 4)))
    group_mix = scatter_about(arg_keys[4], (LAYERS, GROUPS, GROUP, GROUP), GROUP ** -0.5, 0.75)
    w_out = scatter_about(arg_keys[5], (LAYERS, DP, D), DP ** -0.5, 0.1875, ((1, 4), (2, 4)))
    return dict(hidden_in=hidden_in, norm_gain=norm_gain, w_pool_in=w_pool_in, w_pool_gate=w_pool_gate, group_mix=group_mix, w_out=w_out)


norm_eps = 1e-06

def reference(hidden_in, norm_gain, w_pool_in, w_pool_gate, group_mix, w_out):
    resid = hidden_in
    position = jnp.arange(TOKENS, dtype=jnp.int32)
    for layer in range(LAYERS):
        resid_f = resid.astype(jnp.float32)
        mean_sq = lax.optimization_barrier(jnp.mean(resid_f * resid_f, axis=1, keepdims=True))
        normed = (resid_f * lax.rsqrt(mean_sq + norm_eps) * norm_gain[layer]).astype(jnp.bfloat16)
        pool_in = jnp.dot(normed, w_pool_in[layer], preferred_element_type=jnp.float32).astype(jnp.bfloat16)
        gate = jnp.dot(normed, w_pool_gate[layer], preferred_element_type=jnp.float32).astype(jnp.bfloat16)
        grouped = pool_in.astype(jnp.float32).reshape(TOKENS, GROUPS, GROUP)
        running = jnp.concatenate([jnp.zeros((1, GROUPS, GROUP), jnp.float32), jnp.cumsum(grouped, axis=0)], axis=0)
        pieces = []
        for group_id in range(GROUPS):
            half = 2 ** (group_id % 4)
            lower = jnp.clip(position - half, 0, TOKENS).astype(jnp.int32)
            upper = jnp.clip(position + half, 0, TOKENS).astype(jnp.int32)
            window_sum = running[upper, group_id] - running[lower, group_id]
            counted = (upper - lower).astype(jnp.float32)[:, None]
            pieces.append(window_sum / counted - grouped[:, group_id])
        pooled = jnp.stack(pieces, axis=1).astype(jnp.bfloat16)
        mixed = jnp.einsum('tgc,gcd->tgd', pooled.astype(jnp.float32), group_mix[layer].astype(jnp.float32))
        mixed = mixed.reshape(TOKENS, DP)
        branch = (mixed * jax.nn.silu(gate.astype(jnp.float32))).astype(jnp.bfloat16)
        resid = (resid_f + jnp.dot(branch, w_out[layer], preferred_element_type=jnp.float32)).astype(jnp.bfloat16)
    return resid
```

```python
import functools

import jax
import jax.numpy as jnp
from jax import lax
from jax.experimental import pallas as pl
from jax.experimental.pallas import tpu as pltpu
from jax.sharding import PartitionSpec as P

GROUP = 64
HALO = 8
MESH = pl.DeviceIdType.MESH

norm_eps = 1e-06


def mixer(dims, h_in, gain, w_in, w_gate, mix, w_out, out, hg, nb, br, wi, wg, wo, pad, acc_p, acc_g, bd,
          local_sem, zr, zs, yr, ys, gr, gs, pr, ps):
    sp_size, tp_size, layers, rows, cols, chans, chunks = dims
    step_rows = rows // chunks
    chips = tp_size // 2
    half = lax.axis_index("grp")
    row_rank = lax.axis_index("sp")
    rank = lax.axis_index("tp")
    chip, core = rank // 2, lax.rem(rank, 2)
    sibling = chip * 2 + 1 - core
    other = 1 - half
    total_rows = rows * sp_size
    shards = ((w_in, wi), (w_gate, wg), (w_out, wo))

    def chip_rank(distance):
        return lax.rem(chip + distance, chips) * 2 + core

    own_h = pltpu.make_async_copy(h_in, hg.at[0, rank], local_sem.at[0])
    own_h.start()
    own_w = []
    for layer in range(layers):
        for t, (shard, whole) in enumerate(shards):
            depth = shard.shape[1]
            copy = pltpu.make_async_copy(
                shard.at[layer],
                whole.at[layer, pl.ds(pl.multiple_of(row_rank * depth, depth), depth)],
                local_sem.at[1 + layer * 3 + t],
            )
            copy.start()
            own_w.append(copy)

    barrier = pltpu.get_barrier_semaphore()
    peers = [
        {"sp": lax.rem(row_rank + 1, sp_size)},
        {"sp": lax.rem(row_rank + sp_size - 1, sp_size)},
        {"grp": other},
        {"tp": sibling},
    ] + [{"tp": chip_rank(d)} for d in range(1, chips)]
    for peer in peers:
        pl.semaphore_signal(barrier, inc=1, device_id=peer, device_id_type=MESH)
    pl.semaphore_wait(barrier, len(peers))

    def z_copy(layer, t, source, part, to, send):
        shard, whole = shards[t]
        depth = shard.shape[1]
        piece = depth // 2
        start = pl.multiple_of(source * depth + part * piece, piece)
        ref = whole.at[layer, pl.ds(start, piece)]
        return pltpu.make_async_remote_copy(
            ref, ref, zs.at[layer * 3 + t, send], zr.at[layer * 3 + t, source],
            device_id={"sp": to}, device_id_type=MESH,
        )

    def y_copy(layer, t, source, part):
        shard, whole = shards[t]
        depth = shard.shape[1]
        piece = depth // 2
        start = pl.multiple_of(source * depth + part * piece, piece)
        ref = whole.at[layer, pl.ds(start, piece)]
        return pltpu.make_async_remote_copy(
            ref, ref, ys.at[layer * 3 + t, source], yr.at[layer * 3 + t, source],
            device_id={"grp": other}, device_id_type=MESH,
        )

    up = jnp.minimum(row_rank + 1, sp_size - 1)
    down = jnp.maximum(row_rank - 1, 0)

    def z_own(layer):
        for t in range(3):
            @pl.when(row_rank < sp_size - 1)
            def _():
                z_copy(layer, t, row_rank, half, up, row_rank).start()

            @pl.when(row_rank > 0)
            def _():
                z_copy(layer, t, row_rank, half, down, sp_size).start()

    def z_step(layer, distance, t):
        low, high = row_rank - distance, row_rank + distance

        @pl.when(low >= 0)
        def _():
            z_copy(layer, t, low, half, up, low).wait_recv()

            @pl.when(row_rank < sp_size - 1)
            def _():
                z_copy(layer, t, low, half, up, low).start()

            y_copy(layer, t, low, half).start()

        @pl.when(high < sp_size)
        def _():
            z_copy(layer, t, high, half, down, high).wait_recv()

            @pl.when(row_rank > 0)
            def _():
                z_copy(layer, t, high, half, down, high).start()

            y_copy(layer, t, high, half).start()

    def y_arrived(layer, t):
        for source in range(sp_size):
            @pl.when(row_rank != source)
            def _():
                y_copy(layer, t, source, other).wait_recv()

    def weights_sent():
        for layer in range(layers):
            for t in range(3):
                for source in range(sp_size):
                    @pl.when(row_rank != source)
                    def _():
                        y_copy(layer, t, source, half).wait_send()

                    @pl.when((source <= row_rank) & (row_rank < sp_size - 1))
                    def _():
                        z_copy(layer, t, source, half, up, source).wait_send()

                    @pl.when((source > row_rank) & (row_rank > 0))
                    def _():
                        z_copy(layer, t, source, half, down, source).wait_send()

                @pl.when(row_rank > 0)
                def _():
                    z_copy(layer, t, row_rank, half, down, sp_size).wait_send()

    def g_copy(kind, layer, chunk, source, to, send):
        buffer = (hg, br)[kind]
        ref = buffer.at[layer, source, pl.ds(chunk * step_rows, step_rows)]
        index = (kind * layers + layer) * chunks + chunk
        return pltpu.make_async_remote_copy(
            ref, ref, gs.at[index, send], gr.at[index, source], device_id={"tp": to}, device_id_type=MESH
        )

    def g_send(kind, layer, chunk):
        for d in range(1, chips):
            g_copy(kind, layer, chunk, rank, chip_rank(d), d).start()
        g_copy(kind, layer, chunk, rank, sibling, 0).start()

    def g_relay(kind, layer, chunk):
        for d in range(1, chips):
            source = chip_rank(d)
            g_copy(kind, layer, chunk, source, sibling, chips + d - 1).wait_recv()
            g_copy(kind, layer, chunk, source, sibling, chips + d - 1).start()

    def g_arrived(kind, layer, chunk):
        for d in range(chips):
            source = lax.rem(chip + d, chips) * 2 + 1 - core
            g_copy(kind, layer, chunk, source, sibling, 0).wait_recv()

    def g_sent(kind, layer, chunk):
        for d in range(1, chips):
            g_copy(kind, layer, chunk, rank, chip_rank(d), d).wait_send()
            g_copy(kind, layer, chunk, chip_rank(d), sibling, chips + d - 1).wait_send()
        g_copy(kind, layer, chunk, rank, sibling, 0).wait_send()

    def normalize(layer, chunk):
        span = pl.ds(chunk * step_rows, step_rows)
        squares = jnp.zeros((step_rows, 1), jnp.float32)
        for k in range(tp_size):
            block = hg[layer, k, span, :].astype(jnp.float32)
            squares = squares + jnp.sum(block * block, axis=1, keepdims=True)
        scaling = lax.rsqrt(squares / (cols * tp_size) + norm_eps)
        for k in range(tp_size):
            block = hg[layer, k, span, :].astype(jnp.float32)
            own_gain = gain[layer : layer + 1, k * cols : (k + 1) * cols]
            nb[k, span, :] = (block * scaling * own_gain).astype(jnp.bfloat16)

    def project(acc, whole, layer):
        acc[...] = jnp.zeros_like(acc)

        @pl.loop(0, tp_size)
        def _(k):
            weight = whole[layer, pl.ds(pl.multiple_of(k * cols, cols), cols), :]
            acc[...] += jnp.dot(nb[k], weight, preferred_element_type=jnp.float32)

    def halo_copy(layer, upward):
        source, target = (rows, 0) if upward else (HALO, rows + HALO)
        side = 0 if upward else 1
        return pltpu.make_async_remote_copy(
            pad.at[layer, pl.ds(source, HALO)], pad.at[layer, pl.ds(target, HALO)],
            ps.at[layer, side], pr.at[layer, side],
            device_id={"sp": up if upward else down}, device_id_type=MESH,
        )

    def halo_send(layer):
        @pl.when(row_rank < sp_size - 1)
        def _():
            halo_copy(layer, True).start()

        @pl.when(row_rank > 0)
        def _():
            halo_copy(layer, False).start()

    def halo_arrived(layer):
        @pl.when(row_rank > 0)
        def _():
            halo_copy(layer, True).wait_recv()

        @pl.when(row_rank < sp_size - 1)
        def _():
            halo_copy(layer, False).wait_recv()

    def halo_sent(layer):
        @pl.when(row_rank < sp_size - 1)
        def _():
            halo_copy(layer, True).wait_send()

        @pl.when(row_rank > 0)
        def _():
            halo_copy(layer, False).wait_send()

    groups = chans // GROUP

    def mix_matrix(layer):
        for g in range(groups):
            block = mix[layer, rank * groups + g].astype(jnp.float32)
            parts = [block if g == c else jnp.zeros((GROUP, GROUP), jnp.float32) for c in range(groups)]
            wide = parts[0] if groups == 1 else jnp.concatenate(parts, axis=1)
            bd[layer, g * GROUP : (g + 1) * GROUP, :] = wide.astype(jnp.bfloat16)

    def pool_chunk(layer, chunk):
        base = chunk * step_rows
        length = step_rows + 2 * HALO
        x = pad[layer, base : base + length, :]

        def ahead(v, n):
            return pltpu.roll(v, length - n, 0)

        sum1 = x + ahead(x, 1)
        sum2 = sum1 + ahead(sum1, 2)
        sum4 = sum2 + ahead(sum2, 4)
        sum8 = sum4 + ahead(sum4, 8)
        lane = lax.broadcasted_iota(jnp.int32, (step_rows, chans), 1)
        code = lax.rem(rank * groups + lane // GROUP, 4)
        position = row_rank * rows + base + lax.broadcasted_iota(jnp.int32, (step_rows, chans), 0)
        running = jnp.where(
            code == 0, ahead(sum1, 7)[:step_rows],
            jnp.where(
                code == 1, ahead(sum2, 6)[:step_rows],
                jnp.where(code == 2, ahead(sum4, 4)[:step_rows], sum8[:step_rows]),
            ),
        )
        window = jnp.where(code == 0, 1, jnp.where(code == 1, 2, jnp.where(code == 2, 4, 8)))
        counted = (jnp.minimum(position + window, total_rows) - jnp.maximum(position - window, 0)).astype(jnp.float32)
        pooled = (running / counted - x[HALO : HALO + step_rows]).astype(jnp.bfloat16)
        mixed = jnp.dot(pooled, bd[layer], preferred_element_type=jnp.float32)
        gate = acc_g[base : base + step_rows, :].astype(jnp.bfloat16).astype(jnp.float32)
        branch = mixed * (gate / (1.0 + jnp.exp(-gate)))
        br[layer, rank, pl.ds(base, step_rows), :] = branch.astype(jnp.bfloat16)

    def out_chunk(layer, chunk):
        span = pl.ds(chunk * step_rows, step_rows)
        total = hg[layer, rank, span, :].astype(jnp.float32)
        for k in range(tp_size):
            total = total + jnp.dot(
                br[layer, k, span, :], wo[layer, k * chans : (k + 1) * chans, :],
                preferred_element_type=jnp.float32,
            )
        if layer + 1 < layers:
            hg[layer + 1, rank, span, :] = total.astype(jnp.bfloat16)
        else:
            out[span, :] = total.astype(jnp.bfloat16)

    own_h.wait()
    for chunk in range(chunks):
        g_send(0, 0, chunk)
    for copy in own_w:
        copy.wait()
    z_own(0)
    for layer in range(layers):
        mix_matrix(layer)
        for row in (0, rows + HALO):
            @pl.when(row_rank == (0 if row == 0 else sp_size - 1))
            def _():
                pad[layer, row : row + HALO, :] = jnp.zeros((HALO, chans), jnp.float32)

    gather_tasks = [functools.partial(g_relay, 0, 0, chunk) for chunk in range(chunks)]
    weight_tasks = [functools.partial(z_step, 0, d, t) for d in range(1, sp_size) for t in range(3)]

    for layer in range(layers):
        last = layer + 1 == layers
        done = 0
        pairs = max(len(gather_tasks), len(weight_tasks))
        for turn in range(pairs):
            if turn < len(gather_tasks):
                gather_tasks[turn]()
            if turn < len(weight_tasks):
                weight_tasks[turn]()
            if 1 <= turn <= chunks:
                g_arrived(0, layer, turn - 1)
                normalize(layer, turn - 1)
                done = turn
        for chunk in range(done, chunks):
            g_arrived(0, layer, chunk)
            normalize(layer, chunk)
        if not last:
            z_own(layer + 1)
        later = [] if last else [functools.partial(z_step, layer + 1, d, t) for d in range(1, sp_size) for t in range(3)]
        y_arrived(layer, 0)
        project(acc_p, wi, layer)
        pad[layer, HALO : HALO + rows, :] = acc_p[...].astype(jnp.bfloat16).astype(jnp.float32)
        halo_send(layer)
        y_arrived(layer, 1)
        project(acc_g, wg, layer)
        halo_arrived(layer)
        for chunk in range(chunks):
            pool_chunk(layer, chunk)
            g_send(1, layer, chunk)
        for task in later[:1]:
            task()
        for chunk in range(chunks):
            g_relay(1, layer, chunk)
        y_arrived(layer, 2)
        for chunk in range(chunks):
            g_arrived(1, layer, chunk)
            out_chunk(layer, chunk)
            if not last:
                g_send(0, layer + 1, chunk)
        for task in later[1:3]:
            task()
        weight_tasks = later[3:]
        gather_tasks = [] if last else [functools.partial(g_relay, 0, layer + 1, chunk) for chunk in range(chunks)]

    weights_sent()
    for layer in range(layers):
        halo_sent(layer)
        for kind in range(2):
            for chunk in range(chunks):
                g_sent(kind, layer, chunk)


def solution(mesh):
    sp_size, tp_size = mesh.shape["sp"], mesh.shape["tp"]

    def local(hidden_in, norm_gain, w_pool_in, w_pool_gate, group_mix, w_out):
        rows, cols = hidden_in.shape
        layers, _, chans = w_pool_in.shape
        width, channels = cols * tp_size, chans * tp_size
        chunks = rows // 128 if tp_size <= 4 else 1
        dims = (sp_size, tp_size, layers, rows, cols, chans, chunks)
        bf16, f32 = jnp.bfloat16, jnp.float32
        dma = pltpu.SemaphoreType.DMA
        hbm, vmem = pl.BlockSpec(memory_space=pl.ANY), pl.BlockSpec(memory_space=pltpu.VMEM)
        return pl.pallas_call(
            functools.partial(mixer, dims),
            out_shape=jax.ShapeDtypeStruct((rows, cols), bf16),
            in_specs=[hbm, vmem, hbm, hbm, vmem, hbm],
            out_specs=vmem,
            scratch_shapes=[
                pltpu.VMEM((layers, tp_size, rows, cols), bf16),
                pltpu.VMEM((tp_size, rows, cols), bf16),
                pltpu.VMEM((layers, tp_size, rows, chans), bf16),
                pltpu.VMEM((layers, width, chans), bf16),
                pltpu.VMEM((layers, width, chans), bf16),
                pltpu.VMEM((layers, channels, cols), bf16),
                pltpu.VMEM((layers, rows + 2 * HALO, chans), f32),
                pltpu.VMEM((rows, chans), f32),
                pltpu.VMEM((rows, chans), f32),
                pltpu.VMEM((layers, chans, chans), bf16),
                dma((1 + 3 * layers,)),
                dma((3 * layers, sp_size)),
                dma((3 * layers, sp_size + 1)),
                dma((3 * layers, sp_size)),
                dma((3 * layers, sp_size)),
                dma((2 * layers * chunks, tp_size)),
                dma((2 * layers * chunks, tp_size)),
                dma((layers, 2)),
                dma((layers, 2)),
            ],
            compiler_params=pltpu.CompilerParams(
                collective_id=0, has_side_effects=True, vmem_limit_bytes=60 * 1024 * 1024
            ),
        )(hidden_in, norm_gain, w_pool_in, w_pool_gate, group_mix, w_out)

    in_specs = (
        P(("grp", "sp"), "tp"),
        P(),
        P(None, "sp", "tp"),
        P(None, "sp", "tp"),
        P(),
        P(None, "sp", "tp"),
    )
    out_specs = P(("grp", "sp"), "tp")
    return jax.shard_map(local, mesh=mesh, in_specs=in_specs, out_specs=out_specs, check_vma=False)
```

```python
import functools

import jax
import jax.numpy as jnp
from jax import lax
from jax.experimental import pallas as pl
from jax.experimental.pallas import tpu as pltpu
from jax.sharding import PartitionSpec as P

GROUP = 64
HALO = 8
SUBS = 1
AHEAD = 2
START = (0.0, 0.23)
GATHERED = (0.56, 0.78)
POOLED = 0.9
MESH = pl.DeviceIdType.MESH

norm_eps = 1e-06


def mixer(dims, h_in, gain, w_in, w_gate, mix, w_out, out, hg, nb, br, wi, wg, wo, pad, acc_p, acc_g, bd,
          local_sem, zr, zs, yr, ys, gr, gs, pr, ps):
    sp_size, tp_size, layers, rows, cols, chans, chunks = dims
    step_rows = rows // chunks
    chips = tp_size // 2
    half = lax.axis_index("grp")
    row_rank = lax.axis_index("sp")
    rank = lax.axis_index("tp")
    chip, core = rank // 2, lax.rem(rank, 2)
    sibling = chip * 2 + 1 - core
    other = 1 - half
    total_rows = rows * sp_size
    shards = ((w_in, wi), (w_gate, wg), (w_out, wo))

    def chip_rank(distance):
        return lax.rem(chip + distance, chips) * 2 + core

    own_h = pltpu.make_async_copy(h_in, hg.at[0, rank], local_sem.at[0])
    own_h.start()
    own_w = []
    for layer in range(layers):
        for t, (shard, whole) in enumerate(shards):
            depth = shard.shape[1]
            copy = pltpu.make_async_copy(
                shard.at[layer],
                whole.at[layer, pl.ds(pl.multiple_of(row_rank * depth, depth), depth)],
                local_sem.at[1 + layer * 3 + t],
            )
            copy.start()
            own_w.append(copy)

    barrier = pltpu.get_barrier_semaphore()
    peers = [
        {"sp": lax.rem(row_rank + 1, sp_size)},
        {"sp": lax.rem(row_rank + sp_size - 1, sp_size)},
        {"grp": other},
        {"tp": sibling},
    ] + [{"tp": chip_rank(d)} for d in range(1, chips)]
    for peer in peers:
        pl.semaphore_signal(barrier, inc=1, device_id=peer, device_id_type=MESH)
    pl.semaphore_wait(barrier, len(peers))

    pieces = [(layer, t, sub) for layer in range(layers) for t in range(3) for sub in range(SUBS)]

    def piece_ref(q, source, part):
        layer, t, sub = pieces[q]
        shard, whole = shards[t]
        depth = shard.shape[1]
        size = depth // (2 * SUBS)
        start = pl.multiple_of(source * depth + (part * SUBS + sub) * size, size)
        return whole.at[layer, pl.ds(start, size)]

    def z_copy(q, source, to, send):
        ref = piece_ref(q, source, half)
        return pltpu.make_async_remote_copy(
            ref, ref, zs.at[q, send], zr.at[q, source], device_id={"sp": to}, device_id_type=MESH
        )

    def y_copy(q, source, part):
        ref = piece_ref(q, source, part)
        return pltpu.make_async_remote_copy(
            ref, ref, ys.at[q, source], yr.at[q, source], device_id={"grp": other}, device_id_type=MESH
        )

    up = jnp.minimum(row_rank + 1, sp_size - 1)
    down = jnp.maximum(row_rank - 1, 0)

    def z_own(q):
        layer, t, sub = pieces[q]
        if sub == 0:
            own_w[layer * 3 + t].wait()

        @pl.when(row_rank < sp_size - 1)
        def _():
            z_copy(q, row_rank, up, row_rank).start()

        @pl.when(row_rank > 0)
        def _():
            z_copy(q, row_rank, down, sp_size).start()

    def z_step(q, distance):
        low, high = row_rank - distance, row_rank + distance

        @pl.when(low >= 0)
        def _():
            z_copy(q, low, up, low).wait_recv()

            @pl.when(row_rank < sp_size - 1)
            def _():
                z_copy(q, low, up, low).start()

            y_copy(q, low, half).start()

        @pl.when(high < sp_size)
        def _():
            z_copy(q, high, down, high).wait_recv()

            @pl.when(row_rank > 0)
            def _():
                z_copy(q, high, down, high).start()

            y_copy(q, high, half).start()

        if distance == sp_size - 1 and q + AHEAD < len(pieces):
            z_own(q + AHEAD)

    steps = [functools.partial(z_step, q, d) for q in range(len(pieces)) for d in range(1, sp_size)]

    def advance(upto):
        while steps and len(pieces) * (sp_size - 1) - len(steps) < upto:
            steps.pop(0)()

    def y_arrived(layer, t):
        for q, piece in enumerate(pieces):
            if piece[:2] == (layer, t):
                advance((q + 1) * (sp_size - 1))
                for source in range(sp_size):
                    @pl.when(row_rank != source)
                    def _():
                        y_copy(q, source, other).wait_recv()

    def weights_sent():
        for q in range(len(pieces)):
            for source in range(sp_size):
                @pl.when(row_rank != source)
                def _():
                    y_copy(q, source, half).wait_send()

                @pl.when((source <= row_rank) & (row_rank < sp_size - 1))
                def _():
                    z_copy(q, source, up, source).wait_send()

                @pl.when((source > row_rank) & (row_rank > 0))
                def _():
                    z_copy(q, source, down, source).wait_send()

            @pl.when(row_rank > 0)
            def _():
                z_copy(q, row_rank, down, sp_size).wait_send()

    def g_copy(kind, layer, chunk, source, to, send):
        buffer = (hg, br)[kind]
        ref = buffer.at[layer, source, pl.ds(chunk * step_rows, step_rows)]
        index = (kind * layers + layer) * chunks + chunk
        return pltpu.make_async_remote_copy(
            ref, ref, gs.at[index, send], gr.at[index, source], device_id={"tp": to}, device_id_type=MESH
        )

    def g_send(kind, layer, chunk):
        for d in range(1, chips):
            g_copy(kind, layer, chunk, rank, chip_rank(d), d).start()
        g_copy(kind, layer, chunk, rank, sibling, 0).start()

    def g_relay(kind, layer, chunk):
        for d in range(1, chips):
            source = chip_rank(d)
            g_copy(kind, layer, chunk, source, sibling, chips + d - 1).wait_recv()
            g_copy(kind, layer, chunk, source, sibling, chips + d - 1).start()

    def g_arrived(kind, layer, chunk):
        for d in range(chips):
            source = lax.rem(chip + d, chips) * 2 + 1 - core
            g_copy(kind, layer, chunk, source, sibling, 0).wait_recv()

    def g_sent(kind, layer, chunk):
        for d in range(1, chips):
            g_copy(kind, layer, chunk, rank, chip_rank(d), d).wait_send()
            g_copy(kind, layer, chunk, chip_rank(d), sibling, chips + d - 1).wait_send()
        g_copy(kind, layer, chunk, rank, sibling, 0).wait_send()

    def normalize(layer, chunk):
        span = pl.ds(chunk * step_rows, step_rows)
        squares = jnp.zeros((step_rows, 1), jnp.float32)
        for k in range(tp_size):
            block = hg[layer, k, span, :].astype(jnp.float32)
            squares = squares + jnp.sum(block * block, axis=1, keepdims=True)
        scaling = lax.rsqrt(squares / (cols * tp_size) + norm_eps)
        for k in range(tp_size):
            block = hg[layer, k, span, :].astype(jnp.float32)
            own_gain = gain[layer : layer + 1, k * cols : (k + 1) * cols]
            nb[k, span, :] = (block * scaling * own_gain).astype(jnp.bfloat16)

    def project(acc, whole, layer):
        acc[...] = jnp.zeros_like(acc)

        @pl.loop(0, tp_size)
        def _(k):
            weight = whole[layer, pl.ds(pl.multiple_of(k * cols, cols), cols), :]
            acc[...] += jnp.dot(nb[k], weight, preferred_element_type=jnp.float32)

    def halo_copy(layer, upward):
        source, target = (rows, 0) if upward else (HALO, rows + HALO)
        side = 0 if upward else 1
        return pltpu.make_async_remote_copy(
            pad.at[layer, pl.ds(source, HALO)], pad.at[layer, pl.ds(target, HALO)],
            ps.at[layer, side], pr.at[layer, side],
            device_id={"sp": up if upward else down}, device_id_type=MESH,
        )

    def halo_send(layer):
        @pl.when(row_rank < sp_size - 1)
        def _():
            halo_copy(layer, True).start()

        @pl.when(row_rank > 0)
        def _():
            halo_copy(layer, False).start()

    def halo_arrived(layer):
        @pl.when(row_rank > 0)
        def _():
            halo_copy(layer, True).wait_recv()

        @pl.when(row_rank < sp_size - 1)
        def _():
            halo_copy(layer, False).wait_recv()

    def halo_sent(layer):
        @pl.when(row_rank < sp_size - 1)
        def _():
            halo_copy(layer, True).wait_send()

        @pl.when(row_rank > 0)
        def _():
            halo_copy(layer, False).wait_send()

    groups = chans // GROUP

    def mix_matrix(layer):
        for g in range(groups):
            block = mix[layer, rank * groups + g].astype(jnp.float32)
            parts = [block if g == c else jnp.zeros((GROUP, GROUP), jnp.float32) for c in range(groups)]
            wide = parts[0] if groups == 1 else jnp.concatenate(parts, axis=1)
            bd[layer, g * GROUP : (g + 1) * GROUP, :] = wide.astype(jnp.bfloat16)

    def pool_chunk(layer, chunk):
        base = chunk * step_rows
        length = step_rows + 2 * HALO
        x = pad[layer, base : base + length, :]

        def ahead(v, n):
            return pltpu.roll(v, length - n, 0)

        sum1 = x + ahead(x, 1)
        sum2 = sum1 + ahead(sum1, 2)
        sum4 = sum2 + ahead(sum2, 4)
        sum8 = sum4 + ahead(sum4, 8)
        lane = lax.broadcasted_iota(jnp.int32, (step_rows, chans), 1)
        code = lax.rem(rank * groups + lane // GROUP, 4)
        position = row_rank * rows + base + lax.broadcasted_iota(jnp.int32, (step_rows, chans), 0)
        running = jnp.where(
            code == 0, ahead(sum1, 7)[:step_rows],
            jnp.where(
                code == 1, ahead(sum2, 6)[:step_rows],
                jnp.where(code == 2, ahead(sum4, 4)[:step_rows], sum8[:step_rows]),
            ),
        )
        window = jnp.where(code == 0, 1, jnp.where(code == 1, 2, jnp.where(code == 2, 4, 8)))
        counted = (jnp.minimum(position + window, total_rows) - jnp.maximum(position - window, 0)).astype(jnp.float32)
        pooled = (running / counted - x[HALO : HALO + step_rows]).astype(jnp.bfloat16)
        mixed = jnp.dot(pooled, bd[layer], preferred_element_type=jnp.float32)
        gate = acc_g[base : base + step_rows, :].astype(jnp.bfloat16).astype(jnp.float32)
        branch = mixed * (gate / (1.0 + jnp.exp(-gate)))
        br[layer, rank, pl.ds(base, step_rows), :] = branch.astype(jnp.bfloat16)

    def out_chunk(layer, chunk):
        span = pl.ds(chunk * step_rows, step_rows)
        total = hg[layer, rank, span, :].astype(jnp.float32)
        for k in range(tp_size):
            total = total + jnp.dot(
                br[layer, k, span, :], wo[layer, k * chans : (k + 1) * chans, :],
                preferred_element_type=jnp.float32,
            )
        if layer + 1 < layers:
            hg[layer + 1, rank, span, :] = total.astype(jnp.bfloat16)
        else:
            out[span, :] = total.astype(jnp.bfloat16)

    own_h.wait()
    for chunk in range(chunks):
        g_send(0, 0, chunk)
    for q in range(AHEAD):
        z_own(q)
    for layer in range(layers):
        mix_matrix(layer)
        for row in (0, rows + HALO):
            @pl.when(row_rank == (0 if row == 0 else sp_size - 1))
            def _():
                pad[layer, row : row + HALO, :] = jnp.zeros((HALO, chans), jnp.float32)

    per_layer = len(pieces) // layers * (sp_size - 1)

    def pace(layer, part):
        advance(layer * per_layer + int(per_layer * part))

    for layer in range(layers):
        last = layer + 1 == layers
        for chunk in range(chunks):
            g_relay(0, layer, chunk)
            pace(layer, START[layer > 0] + (GATHERED[layer > 0] - START[layer > 0]) * (chunk + 1) / chunks)
            if chunk:
                g_arrived(0, layer, chunk - 1)
                normalize(layer, chunk - 1)
        g_arrived(0, layer, chunks - 1)
        normalize(layer, chunks - 1)
        y_arrived(layer, 0)
        project(acc_p, wi, layer)
        pad[layer, HALO : HALO + rows, :] = acc_p[...].astype(jnp.bfloat16).astype(jnp.float32)
        halo_send(layer)
        y_arrived(layer, 1)
        project(acc_g, wg, layer)
        halo_arrived(layer)
        for chunk in range(chunks):
            pool_chunk(layer, chunk)
            g_send(1, layer, chunk)
        pace(layer, POOLED)
        for chunk in range(chunks):
            g_relay(1, layer, chunk)
        y_arrived(layer, 2)
        for chunk in range(chunks):
            g_arrived(1, layer, chunk)
            out_chunk(layer, chunk)
            if not last:
                g_send(0, layer + 1, chunk)
        if not last:
            pace(layer + 1, START[1])

    weights_sent()
    for layer in range(layers):
        halo_sent(layer)
        for kind in range(2):
            for chunk in range(chunks):
                g_sent(kind, layer, chunk)


def solution(mesh):
    sp_size, tp_size = mesh.shape["sp"], mesh.shape["tp"]

    def local(hidden_in, norm_gain, w_pool_in, w_pool_gate, group_mix, w_out):
        rows, cols = hidden_in.shape
        layers, _, chans = w_pool_in.shape
        width, channels = cols * tp_size, chans * tp_size
        chunks = rows // 128 if tp_size <= 4 else 1
        dims = (sp_size, tp_size, layers, rows, cols, chans, chunks)
        bf16, f32 = jnp.bfloat16, jnp.float32
        dma = pltpu.SemaphoreType.DMA
        hbm, vmem = pl.BlockSpec(memory_space=pl.ANY), pl.BlockSpec(memory_space=pltpu.VMEM)
        return pl.pallas_call(
            functools.partial(mixer, dims),
            out_shape=jax.ShapeDtypeStruct((rows, cols), bf16),
            in_specs=[hbm, vmem, hbm, hbm, vmem, hbm],
            out_specs=vmem,
            scratch_shapes=[
                pltpu.VMEM((layers, tp_size, rows, cols), bf16),
                pltpu.VMEM((tp_size, rows, cols), bf16),
                pltpu.VMEM((layers, tp_size, rows, chans), bf16),
                pltpu.VMEM((layers, width, chans), bf16),
                pltpu.VMEM((layers, width, chans), bf16),
                pltpu.VMEM((layers, channels, cols), bf16),
                pltpu.VMEM((layers, rows + 2 * HALO, chans), f32),
                pltpu.VMEM((rows, chans), f32),
                pltpu.VMEM((rows, chans), f32),
                pltpu.VMEM((layers, chans, chans), bf16),
                dma((1 + 3 * layers,)),
                dma((3 * layers * SUBS, sp_size)),
                dma((3 * layers * SUBS, sp_size + 1)),
                dma((3 * layers * SUBS, sp_size)),
                dma((3 * layers * SUBS, sp_size)),
                dma((2 * layers * chunks, tp_size)),
                dma((2 * layers * chunks, tp_size)),
                dma((layers, 2)),
                dma((layers, 2)),
            ],
            compiler_params=pltpu.CompilerParams(
                collective_id=0, has_side_effects=True, vmem_limit_bytes=60 * 1024 * 1024
            ),
        )(hidden_in, norm_gain, w_pool_in, w_pool_gate, group_mix, w_out)

    in_specs = (
        P(("grp", "sp"), "tp"),
        P(),
        P(None, "sp", "tp"),
        P(None, "sp", "tp"),
        P(),
        P(None, "sp", "tp"),
    )
    out_specs = P(("grp", "sp"), "tp")
    return jax.shard_map(local, mesh=mesh, in_specs=in_specs, out_specs=out_specs, check_vma=False)
```

```python
import functools

import jax
import jax.numpy as jnp
from jax import lax
from jax.experimental import pallas as pl
from jax.experimental.pallas import tpu as pltpu
from jax.sharding import PartitionSpec as P

GROUP = 64
HALO = 8
SUBS = 1
AHEAD = 2
START = (0.0, 0.34)
GATHERED = (0.56, 0.67)
PROJECTED = (0.78, 0.89)
GATED = (0.89, 1.0)
POOLED = (1.0, 1.23)
RELAYED = (1.0, 1.23)
MESH = pl.DeviceIdType.MESH

norm_eps = 1e-06


def mixer(dims, h_in, gain, w_in, w_gate, mix, w_out, out, hg, nb, br, wi, wg, wo, pad, acc_p, acc_g, bd,
          local_sem, zr, zs, yr, ys, gr, gs, pr, ps):
    sp_size, tp_size, layers, rows, cols, chans, chunks = dims
    step_rows = rows // chunks
    chips = tp_size // 2
    half = lax.axis_index("grp")
    row_rank = lax.axis_index("sp")
    rank = lax.axis_index("tp")
    chip, core = rank // 2, lax.rem(rank, 2)
    sibling = chip * 2 + 1 - core
    other = 1 - half
    total_rows = rows * sp_size
    shards = ((w_in, wi), (w_gate, wg), (w_out, wo))

    def chip_rank(distance):
        return lax.rem(chip + distance, chips) * 2 + core

    own_w = []
    for layer in range(layers):
        for t, (shard, whole) in enumerate(shards):
            depth = shard.shape[1]
            copy = pltpu.make_async_copy(
                shard.at[layer],
                whole.at[layer, pl.ds(pl.multiple_of(row_rank * depth, depth), depth)],
                local_sem.at[1 + layer * 3 + t],
            )
            copy.start()
            own_w.append(copy)
    own_h = pltpu.make_async_copy(h_in, hg.at[0, rank], local_sem.at[0])
    own_h.start()

    barrier = pltpu.get_barrier_semaphore()
    peers = [
        {"sp": lax.rem(row_rank + 1, sp_size)},
        {"sp": lax.rem(row_rank + sp_size - 1, sp_size)},
        {"grp": other},
        {"tp": sibling},
    ] + [{"tp": chip_rank(d)} for d in range(1, chips)]
    for peer in peers:
        pl.semaphore_signal(barrier, inc=1, device_id=peer, device_id_type=MESH)
    pl.semaphore_wait(barrier, len(peers))

    pieces = [(layer, t, sub) for layer in range(layers) for t in range(3) for sub in range(SUBS)]
    final = len(pieces) - 1
    extra = final + 1
    pieces.append(pieces[final])
    ends = (0, sp_size - 1)

    def swapped(q, source):
        return q < final or (q == final and source not in ends)

    def piece_ref(q, source, part):
        layer, t, sub = pieces[q]
        shard, whole = shards[t]
        depth = shard.shape[1]
        size = depth // (2 * SUBS)
        start = pl.multiple_of(source * depth + (part * SUBS + sub) * size, size)
        return whole.at[layer, pl.ds(start, size)]

    def z_copy(q, source, to, send):
        ref = piece_ref(q, source, other if q == extra else half)
        return pltpu.make_async_remote_copy(
            ref, ref, zs.at[q, send], zr.at[q, source], device_id={"sp": to}, device_id_type=MESH
        )

    def y_copy(q, source, part):
        ref = piece_ref(q, source, part)
        return pltpu.make_async_remote_copy(
            ref, ref, ys.at[q, source], yr.at[q, source], device_id={"grp": other}, device_id_type=MESH
        )

    up = jnp.minimum(row_rank + 1, sp_size - 1)
    down = jnp.maximum(row_rank - 1, 0)

    def z_own(q):
        layer, t, sub = pieces[q]
        if sub == 0 and q < extra:
            own_w[layer * 3 + t].wait()

        @pl.when((row_rank == 0) if q == extra else (row_rank < sp_size - 1))
        def _():
            z_copy(q, row_rank, up, row_rank).start()

        @pl.when((row_rank == sp_size - 1) if q == extra else (row_rank > 0))
        def _():
            z_copy(q, row_rank, down, sp_size).start()

    def z_step(q, distance):
        low, high = row_rank - distance, row_rank + distance

        @pl.when((low == 0) if q == extra else (low >= 0))
        def _():
            z_copy(q, low, up, low).wait_recv()

            @pl.when(row_rank < sp_size - 1)
            def _():
                z_copy(q, low, up, low).start()

            if q < final:
                y_copy(q, low, half).start()
            elif q == final:
                @pl.when(low > 0)
                def _():
                    y_copy(q, low, half).start()

        @pl.when((high == sp_size - 1) if q == extra else (high < sp_size))
        def _():
            z_copy(q, high, down, high).wait_recv()

            @pl.when(row_rank > 0)
            def _():
                z_copy(q, high, down, high).start()

            if q < final:
                y_copy(q, high, half).start()
            elif q == final:
                @pl.when(high < sp_size - 1)
                def _():
                    y_copy(q, high, half).start()

        if distance == sp_size - 1 and q + AHEAD < len(pieces):
            z_own(q + AHEAD)

    steps = [functools.partial(z_step, q, d) for q in range(len(pieces)) for d in range(1, sp_size)]

    def advance(upto):
        while steps and len(pieces) * (sp_size - 1) - len(steps) < upto:
            steps.pop(0)()

    def y_arrived(layer, t):
        for q, piece in enumerate(pieces):
            if piece[:2] == (layer, t):
                advance((q + 1) * (sp_size - 1))
                for source in range(sp_size):
                    if not swapped(q, source):
                        continue

                    @pl.when(row_rank != source)
                    def _():
                        y_copy(q, source, other).wait_recv()

    def weights_sent():
        for q in range(len(pieces)):
            for source in range(sp_size):
                if swapped(q, source):
                    @pl.when(row_rank != source)
                    def _():
                        y_copy(q, source, half).wait_send()

                if q < extra or source == 0:
                    @pl.when((source <= row_rank) & (row_rank < sp_size - 1))
                    def _():
                        z_copy(q, source, up, source).wait_send()

                if q < extra or source == sp_size - 1:
                    @pl.when((source > row_rank) & (row_rank > 0))
                    def _():
                        z_copy(q, source, down, source).wait_send()

            @pl.when((row_rank == sp_size - 1) if q == extra else (row_rank > 0))
            def _():
                z_copy(q, row_rank, down, sp_size).wait_send()

    def g_copy(kind, layer, chunk, source, to, send):
        buffer = (hg, br)[kind]
        ref = buffer.at[layer, source, pl.ds(chunk * step_rows, step_rows)]
        index = (kind * layers + layer) * chunks + chunk
        return pltpu.make_async_remote_copy(
            ref, ref, gs.at[index, send], gr.at[index, source], device_id={"tp": to}, device_id_type=MESH
        )

    def g_send(kind, layer, chunk):
        for d in range(1, chips):
            g_copy(kind, layer, chunk, rank, chip_rank(d), d).start()
        g_copy(kind, layer, chunk, rank, sibling, 0).start()

    def g_relay(kind, layer, chunk):
        for d in range(1, chips):
            source = chip_rank(d)
            g_copy(kind, layer, chunk, source, sibling, chips + d - 1).wait_recv()
            g_copy(kind, layer, chunk, source, sibling, chips + d - 1).start()

    def g_arrived(kind, layer, chunk):
        for d in range(chips):
            source = lax.rem(chip + d, chips) * 2 + 1 - core
            g_copy(kind, layer, chunk, source, sibling, 0).wait_recv()

    def g_sent(kind, layer, chunk):
        for d in range(1, chips):
            g_copy(kind, layer, chunk, rank, chip_rank(d), d).wait_send()
            g_copy(kind, layer, chunk, chip_rank(d), sibling, chips + d - 1).wait_send()
        g_copy(kind, layer, chunk, rank, sibling, 0).wait_send()

    def normalize(layer, chunk):
        span = pl.ds(chunk * step_rows, step_rows)
        squares = jnp.zeros((step_rows, 1), jnp.float32)
        for k in range(tp_size):
            block = hg[layer, k, span, :].astype(jnp.float32)
            squares = squares + jnp.sum(block * block, axis=1, keepdims=True)
        scaling = lax.rsqrt(squares / (cols * tp_size) + norm_eps)
        for k in range(tp_size):
            block = hg[layer, k, span, :].astype(jnp.float32)
            own_gain = gain[layer : layer + 1, k * cols : (k + 1) * cols]
            nb[k, span, :] = (block * scaling * own_gain).astype(jnp.bfloat16)

    def project(acc, whole, layer):
        acc[...] = jnp.zeros_like(acc)

        @pl.loop(0, tp_size)
        def _(k):
            weight = whole[layer, pl.ds(pl.multiple_of(k * cols, cols), cols), :]
            acc[...] += jnp.dot(nb[k], weight, preferred_element_type=jnp.float32)

    def halo_copy(layer, upward):
        source, target = (rows, 0) if upward else (HALO, rows + HALO)
        side = 0 if upward else 1
        return pltpu.make_async_remote_copy(
            pad.at[layer, pl.ds(source, HALO)], pad.at[layer, pl.ds(target, HALO)],
            ps.at[layer, side], pr.at[layer, side],
            device_id={"sp": up if upward else down}, device_id_type=MESH,
        )

    def halo_send(layer):
        @pl.when(row_rank < sp_size - 1)
        def _():
            halo_copy(layer, True).start()

        @pl.when(row_rank > 0)
        def _():
            halo_copy(layer, False).start()

    def halo_arrived(layer):
        @pl.when(row_rank > 0)
        def _():
            halo_copy(layer, True).wait_recv()

        @pl.when(row_rank < sp_size - 1)
        def _():
            halo_copy(layer, False).wait_recv()

    def halo_sent(layer):
        @pl.when(row_rank < sp_size - 1)
        def _():
            halo_copy(layer, True).wait_send()

        @pl.when(row_rank > 0)
        def _():
            halo_copy(layer, False).wait_send()

    groups = chans // GROUP

    def mix_matrix(layer):
        for g in range(groups):
            block = mix[layer, rank * groups + g].astype(jnp.float32)
            parts = [block if g == c else jnp.zeros((GROUP, GROUP), jnp.float32) for c in range(groups)]
            wide = parts[0] if groups == 1 else jnp.concatenate(parts, axis=1)
            bd[layer, g * GROUP : (g + 1) * GROUP, :] = wide.astype(jnp.bfloat16)

    def pool_chunk(layer, chunk):
        base = chunk * step_rows
        length = step_rows + 2 * HALO
        x = pad[layer, base : base + length, :]

        def ahead(v, n):
            return pltpu.roll(v, length - n, 0)

        sum1 = x + ahead(x, 1)
        sum2 = sum1 + ahead(sum1, 2)
        sum4 = sum2 + ahead(sum2, 4)
        sum8 = sum4 + ahead(sum4, 8)
        lane = lax.broadcasted_iota(jnp.int32, (step_rows, chans), 1)
        code = lax.rem(rank * groups + lane // GROUP, 4)
        position = row_rank * rows + base + lax.broadcasted_iota(jnp.int32, (step_rows, chans), 0)
        running = jnp.where(
            code == 0, ahead(sum1, 7)[:step_rows],
            jnp.where(
                code == 1, ahead(sum2, 6)[:step_rows],
                jnp.where(code == 2, ahead(sum4, 4)[:step_rows], sum8[:step_rows]),
            ),
        )
        window = jnp.where(code == 0, 1, jnp.where(code == 1, 2, jnp.where(code == 2, 4, 8)))
        counted = (jnp.minimum(position + window, total_rows) - jnp.maximum(position - window, 0)).astype(jnp.float32)
        pooled = (running / counted - x[HALO : HALO + step_rows]).astype(jnp.bfloat16)
        mixed = jnp.dot(pooled, bd[layer], preferred_element_type=jnp.float32)
        gate = acc_g[base : base + step_rows, :].astype(jnp.bfloat16).astype(jnp.float32)
        branch = mixed * (gate / (1.0 + jnp.exp(-gate)))
        br[layer, rank, pl.ds(base, step_rows), :] = branch.astype(jnp.bfloat16)

    def out_chunk(layer, chunk):
        span = pl.ds(chunk * step_rows, step_rows)
        total = hg[layer, rank, span, :].astype(jnp.float32)
        for k in range(tp_size):
            total = total + jnp.dot(
                br[layer, k, span, :], wo[layer, k * chans : (k + 1) * chans, :],
                preferred_element_type=jnp.float32,
            )
        if layer + 1 < layers:
            hg[layer + 1, rank, span, :] = total.astype(jnp.bfloat16)
        else:
            out[span, :] = total.astype(jnp.bfloat16)

    z_own(0)
    own_h.wait()
    for chunk in range(chunks):
        g_send(0, 0, chunk)
    for q in range(1, AHEAD):
        z_own(q)
    for layer in range(layers):
        mix_matrix(layer)
        for row in (0, rows + HALO):
            @pl.when(row_rank == (0 if row == 0 else sp_size - 1))
            def _():
                pad[layer, row : row + HALO, :] = jnp.zeros((HALO, chans), jnp.float32)

    per_layer = extra // layers * (sp_size - 1)

    def pace(layer, part):
        advance(layer * per_layer + int(per_layer * part + 0.1))

    for layer in range(layers):
        last = layer + 1 == layers
        for chunk in range(chunks):
            g_relay(0, layer, chunk)
            pace(layer, START[layer > 0] + (GATHERED[layer > 0] - START[layer > 0]) * (chunk + 1) / chunks)
            if chunk:
                g_arrived(0, layer, chunk - 1)
                normalize(layer, chunk - 1)
        g_arrived(0, layer, chunks - 1)
        normalize(layer, chunks - 1)
        y_arrived(layer, 0)
        project(acc_p, wi, layer)
        pad[layer, HALO : HALO + rows, :] = acc_p[...].astype(jnp.bfloat16).astype(jnp.float32)
        halo_send(layer)
        pace(layer, PROJECTED[layer > 0])
        y_arrived(layer, 1)
        project(acc_g, wg, layer)
        pace(layer, GATED[layer > 0])
        halo_arrived(layer)
        for chunk in range(chunks):
            pool_chunk(layer, chunk)
            g_send(1, layer, chunk)
        pace(layer, POOLED[layer > 0])
        for chunk in range(chunks):
            g_relay(1, layer, chunk)
        pace(layer, RELAYED[layer > 0])
        y_arrived(layer, 2)
        for chunk in range(chunks):
            g_arrived(1, layer, chunk)
            out_chunk(layer, chunk)
            if not last:
                g_send(0, layer + 1, chunk)
                pace(layer + 1, START[1] * chunk / chunks)
        if not last:
            pace(layer + 1, START[1])

    weights_sent()
    for layer in range(layers):
        halo_sent(layer)
        for kind in range(2):
            for chunk in range(chunks):
                g_sent(kind, layer, chunk)


def solution(mesh):
    sp_size, tp_size = mesh.shape["sp"], mesh.shape["tp"]

    def local(hidden_in, norm_gain, w_pool_in, w_pool_gate, group_mix, w_out):
        rows, cols = hidden_in.shape
        layers, _, chans = w_pool_in.shape
        width, channels = cols * tp_size, chans * tp_size
        chunks = rows // 128 if tp_size <= 4 else 1
        dims = (sp_size, tp_size, layers, rows, cols, chans, chunks)
        bf16, f32 = jnp.bfloat16, jnp.float32
        dma = pltpu.SemaphoreType.DMA
        hbm, vmem = pl.BlockSpec(memory_space=pl.ANY), pl.BlockSpec(memory_space=pltpu.VMEM)
        return pl.pallas_call(
            functools.partial(mixer, dims),
            out_shape=jax.ShapeDtypeStruct((rows, cols), bf16),
            in_specs=[hbm, vmem, hbm, hbm, vmem, hbm],
            out_specs=vmem,
            scratch_shapes=[
                pltpu.VMEM((layers, tp_size, rows, cols), bf16),
                pltpu.VMEM((tp_size, rows, cols), bf16),
                pltpu.VMEM((layers, tp_size, rows, chans), bf16),
                pltpu.VMEM((layers, width, chans), bf16),
                pltpu.VMEM((layers, width, chans), bf16),
                pltpu.VMEM((layers, channels, cols), bf16),
                pltpu.VMEM((layers, rows + 2 * HALO, chans), f32),
                pltpu.VMEM((rows, chans), f32),
                pltpu.VMEM((rows, chans), f32),
                pltpu.VMEM((layers, chans, chans), bf16),
                dma((1 + 3 * layers,)),
                dma((3 * layers * SUBS + 1, sp_size)),
                dma((3 * layers * SUBS + 1, sp_size + 1)),
                dma((3 * layers * SUBS + 1, sp_size)),
                dma((3 * layers * SUBS + 1, sp_size)),
                dma((2 * layers * chunks, tp_size)),
                dma((2 * layers * chunks, tp_size)),
                dma((layers, 2)),
                dma((layers, 2)),
            ],
            compiler_params=pltpu.CompilerParams(
                collective_id=0, has_side_effects=True, vmem_limit_bytes=60 * 1024 * 1024
            ),
        )(hidden_in, norm_gain, w_pool_in, w_pool_gate, group_mix, w_out)

    in_specs = (
        P(("grp", "sp"), "tp"),
        P(),
        P(None, "sp", "tp"),
        P(None, "sp", "tp"),
        P(),
        P(None, "sp", "tp"),
    )
    out_specs = P(("grp", "sp"), "tp")
    return jax.shard_map(local, mesh=mesh, in_specs=in_specs, out_specs=out_specs, check_vma=False)
```
